256 devices in a mesh: grp: 2 (over y), fs: 32 (over z, core), tp: 4 (over x).
Axes of the slice: x: 4, y: 2, z: 16, core: 2. Of those that a mesh axis runs over, the one named last changes fastest.
The devices are a block of a 4x16x16 slice.
Arguments:
- prompt: bfloat16 [8, 1024, 2048], P(('grp', 'tp')), parts along dimension 0, may hold values from -6 to 6
- gate_first: float32 [2048, 5632], P('fs', 'tp'), may hold values from -0.125 to 0.125
- up_first: float32 [2048, 5632], P('fs', 'tp'), may hold values from -0.125 to 0.125
- down_first: float32 [5632, 2048], P('fs', 'tp'), may hold values from -0.3125 to 0.3125
- norm_gain: float32 [2048], replicated, may hold values from 0.1 to 1.9
- gate_second: float32 [2048, 5632], P('fs', 'tp'), may hold values from -0.125 to 0.125
- up_second: float32 [2048, 5632], P('fs', 'tp'), may hold values from -0.125 to 0.125
- down_second: float32 [5632, 2048], P('fs', 'tp'), may hold values from -0.3125 to 0.3125
Outputs:
- result: bfloat16 [8, 1024, 2048], P(('grp', 'tp'), 'fs'), parts along dimension 0
- gate_one: bfloat16 [4096, 5632], P('grp', 'fs'), parts along dimension 0
- up_one: bfloat16 [4096, 5632], P('grp', 'fs'), parts along dimension 0
- down_one: bfloat16 [5632, 4096], P('fs', 'grp'), parts along dimension 1
- gate_two: bfloat16 [4096, 5632], P('grp', 'fs'), parts along dimension 0
- up_two: bfloat16 [4096, 5632], P('grp', 'fs'), parts along dimension 0
- down_two: bfloat16 [5632, 4096], P('fs', 'grp'), parts along dimension 1
The draws below stay inside these ranges and needn't reach their ends.
There are 2 independent parts, one for each index of `grp`. The reference program is written for one: setup_inputs(seed, part) draws one part's arguments, and reference() takes and returns one part's arrays. A program takes and returns all parts, laid end to end along the dimension named above; an argument that names none is the same for every part. Nothing has to cross between parts.
All inputs are finite; a program needn't handle non-finite values.
Results may differ from the reference program's by a relative error of at most 0.029.
Values may be sent and summed in bfloat16 or wider, within the bound.
A program may use at most 64 MiB of HBM per device.

```python
import jax
import jax.numpy as jnp
from jax import lax

D = 2048
FF = 5632
LENGTH = 1024
PROMPTS = 4
N_FS = 32


def block_levels(rng, shape, pieces, least, largest):
    factor_of = 1.0
    for axis_at, blocks in pieces:
        heights = jax.random.uniform(jax.random.fold_in(jax.random.fold_in(rng, 6), axis_at), (blocks,), jnp.float32, least / len(pieces), largest / len(pieces))
        factor_of = factor_of * jnp.repeat(jnp.exp(heights), shape[axis_at] // blocks).reshape((-1,) + (1,) * (len(shape) - 1 - axis_at))
    return factor_of


def bell_draw(key, extent, scale, bound, shards=(), kind=jnp.bfloat16):
    loudness = block_levels(key, extent, shards, -0.22, 0.18) if shards else 1.0
    entries = jax.random.normal(key, extent, jnp.float32) * scale * loudness
    return jnp.minimum(jnp.maximum(entries, -bound), bound).astype(kind)


def setup_inputs(seed: int = 0, part: int = 0) -> dict:
    seeds = jax.random.split(jax.random.key(seed), 9)
    part_keys = jax.random.split(jax.random.fold_in(seeds[8], part), 9)
    prompt = bell_draw(part_keys[0], (PROMPTS, LENGTH, D), 1.0, 6.0, ((0, 4),))
    gate_first = bell_draw(seeds[1], (D, FF), D ** -0.5, 0.125, ((0, 32), (1, 4)), jnp.float32)
    up_first = bell_draw(seeds[2], (D, FF), D ** -0.5, 0.125, ((0, 32), (1, 4)), jnp.float32)
    down_first = bell_draw(seeds[3], (FF, D), (4.0 * FF ** -0.5), 0.3125, ((0, 32), (1, 4)), jnp.float32)
    norm_gain = jnp.clip(1.0 + 0.18 * jax.random.normal(seeds[4], (D,), jnp.float32), 0.1, 1.9)
    gate_second = bell_draw(seeds[5], (D, FF), D ** -0.5, 0.125, ((0, 32), (1, 4)), jnp.float32)
    up_second = bell_draw(seeds[6], (D, FF), D ** -0.5, 0.125, ((0, 32), (1, 4)), jnp.float32)
    down_second = bell_draw(seeds[7], (FF, D), (4.0 * FF ** -0.5), 0.3125, ((0, 32), (1, 4)), jnp.float32)
    return dict(prompt=prompt, gate_first=gate_first, up_first=up_first, down_first=down_first, norm_gain=norm_gain, gate_second=gate_second, up_second=up_second, down_second=down_second)


norm_eps = 1e-05
deep_alpha = 2.0 ** 0.25
half_step = 0.5

def plain_norm(values):
    row_mean = lax.optimization_barrier(jnp.mean(values, axis=-1, keepdims=True))
    centred = values - row_mean
    variance = lax.optimization_barrier(jnp.mean(centred * centred, axis=-1, keepdims=True))
    return centred * lax.rsqrt(variance + norm_eps)

def gated_hidden(inputs, gate_proj, up_proj):
    gate_act = jnp.dot(inputs, gate_proj, preferred_element_type=jnp.float32)
    up_act = jnp.dot(inputs, up_proj, preferred_element_type=jnp.float32)
    return (jax.nn.silu(gate_act) * up_act).astype(jnp.bfloat16)

def block_sums(hidden, down_proj):
    block_width = hidden.shape[1] // N_FS

    def one_block(carried, block_index):
        hidden_block = lax.dynamic_slice_in_dim(hidden, block_index * block_width, block_width, 1)
        down_block = lax.dynamic_slice_in_dim(down_proj, block_index * block_width, block_width, 0)
        partial_term = jnp.dot(hidden_block, down_block, preferred_element_type=jnp.float32).astype(jnp.bfloat16)
        partial_term = lax.optimization_barrier(partial_term)
        return (carried + partial_term.astype(jnp.float32), None)
    start_sum = jnp.zeros((hidden.shape[0], down_proj.shape[1]), jnp.float32)
    summed, unused = lax.scan(one_block, start_sum, jnp.arange(N_FS, dtype=jnp.int32))
    return summed

def reference(prompt, gate_first, up_first, down_first, norm_gain, gate_second, up_second, down_second):
    gate_one = gate_first.astype(jnp.bfloat16)
    up_one = up_first.astype(jnp.bfloat16)
    down_one = down_first.astype(jnp.bfloat16)
    gate_two = (norm_gain[:, None] * gate_second).astype(jnp.bfloat16)
    up_two = (norm_gain[:, None] * up_second).astype(jnp.bfloat16)
    down_two = down_second.astype(jnp.bfloat16)
    tokens = prompt.reshape(-1, prompt.shape[-1])
    hidden_one = gated_hidden(tokens, gate_one, up_one)
    ffn_one = block_sums(hidden_one, down_one)
    normed_one = plain_norm(deep_alpha * tokens.astype(jnp.float32) + half_step * ffn_one).astype(jnp.bfloat16)
    hidden_two = gated_hidden(normed_one, gate_two, up_two)
    ffn_two = block_sums(hidden_two, down_two)
    residual_two = deep_alpha * norm_gain * normed_one.astype(jnp.float32)
    result = plain_norm(residual_two + half_step * ffn_two).astype(jnp.bfloat16).reshape(prompt.shape)
    return (result, gate_one, up_one, down_one, gate_two, up_two, down_two)
```

```python
import functools

import jax
import jax.numpy as jnp
from jax import lax
from jax.experimental import pallas as pl
from jax.experimental.pallas import tpu as pltpu
from jax.sharding import PartitionSpec as P

norm_eps = 1e-05
deep_alpha = 2.0**0.25
half_step = 0.5

LANES = 128
SUBS = 4
TILE_Z = 4
MESH = pl.DeviceIdType.MESH


def plain_norm(values):
    row_mean = jnp.mean(values, axis=-1, keepdims=True)
    centred = values - row_mean
    variance = jnp.mean(centred * centred, axis=-1, keepdims=True)
    return centred * lax.rsqrt(variance + norm_eps)


def split_widths(width):
    main = width // LANES * LANES
    tail = width - main
    return main, tail, -(-2 * tail // LANES) * LANES


def pack_pair(gate, up, tp_size, served):
    rows = gate.shape[0]
    gate = gate.reshape(rows, served, -1)
    up = up.reshape(rows, served, -1)
    main, tail, tail_room = split_widths(gate.shape[-1])
    pieces = [gate[..., :main], up[..., :main], gate[..., main:], up[..., main:]]
    pieces.append(jnp.zeros((rows, served, tail_room - 2 * tail), gate.dtype))
    packed = jnp.concatenate(pieces, axis=-1)
    packed = packed.reshape(tp_size, rows // tp_size, served, packed.shape[-1])
    return packed.transpose(0, 2, 1, 3)


def unpack_pair(packed, width):
    main, tail, _ = split_widths(width)
    packed = packed.reshape(-1, packed.shape[-1])
    gate = jnp.concatenate([packed[:, :main], packed[:, 2 * main : 2 * main + tail]], axis=-1)
    up = jnp.concatenate(
        [packed[:, main : 2 * main], packed[:, 2 * main + tail : 2 * main + 2 * tail]], axis=-1
    )
    return gate, up


def kernel(
    n_fs,
    n_tp,
    width,
    x_in,
    gain,
    src1,
    src2,
    dsrc1,
    dsrc2,
    res_out,
    gu1_out,
    gu2_out,
    dn1_out,
    dn2_out,
    x1,
    x2,
    st1,
    st2,
    gu1,
    gu2,
    dn1,
    dn2,
    part1,
    part2,
    xch1,
    xch2,
    ring1,
    ring2,
    loc_sem,
    out_sem,
    p1_recv,
    p2_recv,
    p3_recv,
    dn_recv,
    xch_recv,
    rs_recv,
    ag_recv,
    sib_recv,
    send_sem,
):
    n_z = n_fs // 2
    half = n_z // 2
    served = n_fs // n_tp
    main, tail, tail_room = split_widths(width)
    me = lax.axis_index("fs")
    me_x = lax.axis_index("tp")
    z, c = me // 2, lax.rem(me, 2)
    sib = me + 1 - 2 * c
    x_right, x_left = lax.rem(me_x + 1, n_tp), lax.rem(me_x + n_tp - 1, n_tp)
    z_right = 2 * lax.rem(z + 1, n_z) + c
    z_left = 2 * lax.rem(z + n_z - 1, n_z) + c
    own, features = x1.shape[2], x1.shape[3]
    sub = features // SUBS
    dcols = dsrc1.shape[1]
    d_cut = width // 32 * 16 + 16

    def remote(src, dst, send, recv, **device):
        return pltpu.make_async_remote_copy(
            src_ref=src, dst_ref=dst, send_sem=send, recv_sem=recv, device_id=device, device_id_type=MESH
        )

    def wait_for(ref, sem):
        pltpu.make_async_copy(ref, ref, sem).wait()

    def d_at(ref, col_block, first=0, size=width):
        return ref.at[pl.ds(first, size), pl.ds(pl.multiple_of(col_block * dcols, dcols), dcols)]

    local = [
        pltpu.make_async_copy(src1.at[me_x], st1.at[me_x], loc_sem.at[0]),
        pltpu.make_async_copy(src2.at[me_x], st2.at[me_x], loc_sem.at[1]),
        pltpu.make_async_copy(dsrc1, d_at(dn1, me_x), loc_sem.at[2]),
        pltpu.make_async_copy(dsrc2, d_at(dn2, me_x), loc_sem.at[3]),
        pltpu.make_async_copy(x_in, x1, loc_sem.at[4]),
    ]
    for copy in local:
        copy.start()

    barrier = pltpu.get_barrier_semaphore()

    def greet_fs(i, carry):
        pl.semaphore_signal(barrier, inc=1, device_id={"fs": lax.rem(me + i, n_fs)}, device_id_type=MESH)
        return carry

    def greet_tp(i, carry):
        pl.semaphore_signal(barrier, inc=1, device_id={"tp": lax.rem(me_x + i, n_tp)}, device_id_type=MESH)
        return carry

    lax.fori_loop(1, n_tp, greet_tp, 0)
    lax.fori_loop(1, n_fs, greet_fs, 0)
    pl.semaphore_wait(barrier, n_fs - 1 + n_tp - 1)

    def scatter_tp(b, src, st):
        for i in range(1, n_tp):
            to = lax.rem(me_x + i, n_tp)
            remote(src.at[to], st.at[me_x], send_sem.at[b, 0], p1_recv.at[b, n_tp - i - 1], tp=to).start()

    def wait_scatter(b, st):
        for i in range(1, n_tp):
            frm = lax.rem(me_x + i, n_tp)
            wait_for(st.at[frm], p1_recv.at[b, i - 1])

    def down_own(b, dsrc, dn):
        remote(dsrc, d_at(dn, me_x), send_sem.at[b, 1], dn_recv.at[b, 0], tp=x_right).start()
        remote(dsrc, d_at(dn, me_x), send_sem.at[b, 2], dn_recv.at[b, 1], tp=x_left).start()

    def down_forward(b, dn):
        wait_for(d_at(dn, x_left), dn_recv.at[b, 0])
        upper = d_at(dn, x_left, 0, d_cut)
        remote(upper, upper, send_sem.at[b, 3], dn_recv.at[b, 2], tp=x_right).start()
        wait_for(d_at(dn, x_right), dn_recv.at[b, 1])
        lower = d_at(dn, x_right, d_cut, width - d_cut)
        remote(lower, lower, send_sem.at[b, 4], dn_recv.at[b, 3], tp=x_left).start()

    def down_wait(b, dn):
        across = lax.rem(me_x + 2, n_tp)
        wait_for(d_at(dn, across, 0, d_cut), dn_recv.at[b, 2])
        wait_for(d_at(dn, across, d_cut, width - d_cut), dn_recv.at[b, 3])

    def at_distance(i):
        reach = (i + 1) // 2
        return lax.rem(z + n_z + reach * (2 * lax.rem(i, 2) - 1), n_z)

    def spread_fs(b, st, gu):
        gu[z, c, me_x] = st[me // served, lax.rem(me, served)]
        remote(
            st.at[sib // served, lax.rem(sib, served)], gu.at[z, c, me_x], send_sem.at[b, 5], p2_recv.at[b, z], fs=sib
        ).start()

        def to_chip(i, carry):
            zi = at_distance(i)
            for other in range(2):
                to = 2 * zi + other
                remote(
                    st.at[to // served, lax.rem(to, served)],
                    gu.at[z, c, me_x],
                    send_sem.at[b, 5],
                    p2_recv.at[b, z],
                    fs=to,
                ).start()
            return carry

        lax.fori_loop(1, n_z, to_chip, 0)

    def gather_own(b, gu, i):
        zi = at_distance(i)
        piece = gu.at[zi, :, me_x]
        remote(piece, piece, send_sem.at[b, 6], p3_recv.at[b, 0, i], tp=x_right).start()
        remote(piece, piece, send_sem.at[b, 7], p3_recv.at[b, 1, i], tp=x_left).start()

    def gather_own_first(b, gu):
        wait_for(gu.at[z, 1 - c, me_x], p2_recv.at[b, z])
        gather_own(b, gu, 0)

    def gather_own_next(b, gu, i):
        zi = at_distance(i)
        wait_for(gu.at[zi, :, me_x], p2_recv.at[b, zi])
        gather_own(b, gu, i)

    def gather_forward(b, gu, i):
        zi = at_distance(i)
        from_left, from_right = gu.at[zi, :, x_left], gu.at[zi, :, x_right]
        wait_for(from_left, p3_recv.at[b, 0, i])
        wait_for(from_right, p3_recv.at[b, 1, i])

        @pl.when(lax.rem(i, 2) == 0)
        def _():
            remote(from_left, from_left, send_sem.at[b, 8], p3_recv.at[b, 2, i], tp=x_right).start()

        @pl.when(lax.rem(i, 2) == 1)
        def _():
            remote(from_right, from_right, send_sem.at[b, 8], p3_recv.at[b, 2, i], tp=x_left).start()

    def gather_wait(b, gu):
        across = lax.rem(me_x + 2, n_tp)

        def one(i, carry):
            wait_for(gu.at[at_distance(i), :, across], p3_recv.at[b, 2, i])
            return carry

        lax.fori_loop(0, n_z, one, 0)

    lag = 2

    def gather_tp(b, gu):
        gather_own_first(b, gu)

        def one(i, carry):
            gather_own_next(b, gu, i)

            @pl.when(i >= lag)
            def _():
                gather_forward(b, gu, i - lag)

            return carry

        lax.fori_loop(1, n_z, one, 0)
        for i in range(n_z - lag, n_z):
            gather_forward(b, gu, jnp.int32(i))

    def compute(b, x, gu, dn, part, xch):
        n_tiles = n_z // TILE_Z
        rows = TILE_Z * 2 * own
        weights = gu[...].reshape(features, gu.shape[-1])

        def tile(i, carry):
            t = lax.rem(z // TILE_Z + n_tiles // 2 + i, n_tiles)
            tokens = x[pl.ds(t * TILE_Z, TILE_Z)].reshape(rows, features)
            act = jnp.dot(tokens, weights, preferred_element_type=jnp.float32)
            gate_main, up_main = act[:, :main], act[:, main : 2 * main]
            rest = act[:, 2 * main :]
            up_rest = pltpu.roll(rest, tail_room - tail, 1)
            lane = lax.broadcasted_iota(jnp.int32, rest.shape, 1)
            rest = jnp.where(lane < tail, jax.nn.silu(rest) * up_rest, 0.0)
            hidden = jnp.concatenate([jax.nn.silu(gate_main) * up_main, rest], axis=1).astype(jnp.bfloat16)
            for k in range(SUBS):
                cols = slice(k * sub, (k + 1) * sub)
                out = jnp.dot(hidden, dn[:, cols], preferred_element_type=jnp.float32)
                part[pl.ds(t * TILE_Z, TILE_Z), :, :, cols] = out.astype(jnp.bfloat16).reshape(
                    TILE_Z, 2, own, sub
                )

            def swap(j, carry):
                zj = t * TILE_Z + j
                remote(part.at[zj, 1 - c], xch.at[zj], send_sem.at[b, 9], xch_recv.at[b, zj], fs=sib).start()
                return carry

            lax.fori_loop(0, TILE_Z, swap, 0)
            return carry

        lax.fori_loop(0, n_tiles, tile, 0)

    def sub_of(ref, k):
        return ref.at[:, pl.ds(k * sub, sub)]

    def reduce_step(b, part, xch, ring, s, both):
        o_right = lax.rem(z + half - s + n_z, n_z)
        o_left = lax.rem(z - (half - 1) + s + 2 * n_z, n_z)
        ways = [(0, o_right, z_right, 0), (1, o_left, z_left, half)][: 2 if both else 1]
        for way, o, to, base in ways:
            wait_for(xch.at[o], xch_recv.at[b, o])
        for k in range(SUBS):
            cols = slice(k * sub, (k + 1) * sub)
            for way, o, to, base in ways:
                total = part[o, c, :, cols].astype(jnp.float32) + xch[o, :, cols].astype(jnp.float32)
                if not isinstance(s, int):
                    wait_for(sub_of(ring.at[base + s - 1], k), rs_recv.at[b, way, s - 1, k])
                    total = total + ring[base + s - 1, :, cols].astype(jnp.float32)
                part[o, c, :, cols] = total.astype(jnp.bfloat16)
                remote(
                    sub_of(part.at[o, c], k),
                    sub_of(ring.at[base + s], k),
                    send_sem.at[b, 10],
                    rs_recv.at[b, way, s, k],
                    fs=to,
                ).start()

    def reduce_rest(b, part, xch, ring):
        def one(s, carry):
            reduce_step(b, part, xch, ring, s, True)
            return carry

        lax.fori_loop(1, half - 1, one, 0)
        reduce_step(b, part, xch, ring, jnp.int32(half - 1), False)

    def reduced_own(b, part, xch, ring):
        wait_for(xch.at[z], xch_recv.at[b, z])
        for k in range(SUBS):
            wait_for(sub_of(ring.at[half - 1], k), rs_recv.at[b, 0, half - 1, k])
            wait_for(sub_of(ring.at[2 * half - 2], k), rs_recv.at[b, 1, half - 2, k])
        pieces = [part[z, c], xch[z], ring[half - 1], ring[2 * half - 2]]
        return sum(p.astype(jnp.float32) for p in pieces)

    def to_sibling(zi):
        chunk = x2.at[zi, c]
        remote(chunk, chunk, send_sem.at[1, 11], sib_recv.at[zi], fs=sib).start()

    def share_step(s, first, left):
        z_from_left = lax.rem(z - s + 2 * n_z, n_z)
        z_from_right = lax.rem(z + s, n_z)
        for k in range(SUBS):
            for way, zi, to, send in [(0, z_from_left, z_right, True), (1, z_from_right, z_left, left)]:
                chunk = sub_of(x2.at[zi, c], k)
                if not first:
                    wait_for(chunk, ag_recv.at[way, s - 1, k])
                if send:
                    remote(chunk, chunk, send_sem.at[0, 11], ag_recv.at[way, s, k], fs=to).start()
        if first:
            to_sibling(z)
        else:
            to_sibling(z_from_left)
            to_sibling(z_from_right)

    def share_tokens():
        share_step(0, True, True)

        def one(s, carry):
            share_step(s, False, True)
            return carry

        lax.fori_loop(1, half - 1, one, 0)
        share_step(jnp.int32(half - 1), False, False)
        far = lax.rem(z + half, n_z)
        for k in range(SUBS):
            wait_for(sub_of(x2.at[far, c], k), ag_recv.at[0, half - 1, k])
        to_sibling(far)

        def sibling_done(zi, carry):
            wait_for(x2.at[zi, 1 - c], sib_recv.at[zi])
            return carry

        lax.fori_loop(0, n_z, sibling_done, 0)

    for copy in local[2:4]:
        copy.wait()
    for dn in (dn1, dn2):
        dn[width:, :] = jnp.zeros((dn.shape[0] - width, features), jnp.bfloat16)

    scatter_tp(0, src1, st1)
    scatter_tp(1, src2, st2)
    down_own(0, dsrc1, dn1)
    local[0].wait()
    wait_scatter(0, st1)
    spread_fs(0, st1, gu1)
    local[1].wait()
    wait_scatter(1, st2)
    spread_fs(1, st2, gu2)
    down_forward(0, dn1)
    gather_tp(0, gu1)
    gather_wait(0, gu1)
    down_wait(0, dn1)
    outs = [
        pltpu.make_async_copy(gu1, gu1_out, out_sem.at[0]),
        pltpu.make_async_copy(dn1.at[pl.ds(0, width)], dn1_out, out_sem.at[1]),
    ]
    for copy in outs:
        copy.start()
    down_own(1, dsrc2, dn2)
    local[4].wait()
    compute(0, x1, gu1, dn1, part1, xch1)
    reduce_step(0, part1, xch1, ring1, 0, True)
    gather_tp(1, gu2)
    down_forward(1, dn2)
    reduce_rest(0, part1, xch1, ring1)
    ffn_one = reduced_own(0, part1, xch1, ring1)
    normed = plain_norm(deep_alpha * x1[z, c].astype(jnp.float32) + half_step * ffn_one)
    x2[z, c] = normed.astype(jnp.bfloat16)
    share_tokens()
    gather_wait(1, gu2)
    down_wait(1, dn2)
    more = [
        pltpu.make_async_copy(gu2, gu2_out, out_sem.at[2]),
        pltpu.make_async_copy(dn2.at[pl.ds(0, width)], dn2_out, out_sem.at[3]),
    ]
    for copy in more:
        copy.start()
    compute(1, x2, gu2, dn2, part2, xch2)
    reduce_step(1, part2, xch2, ring2, 0, True)
    reduce_rest(1, part2, xch2, ring2)
    ffn_two = reduced_own(1, part2, xch2, ring2)
    residual = deep_alpha * gain[...] * x2[z, c].astype(jnp.float32)
    res_out[...] = plain_norm(residual + half_step * ffn_two).astype(jnp.bfloat16)

    for copy in outs + more:
        copy.wait()
    for b, src, st, gu, dsrc, dn, xch, ring in (
        (0, src1, st1, gu1, dsrc1, dn1, xch1, ring1),
        (1, src2, st2, gu2, dsrc2, dn2, xch2, ring2),
    ):
        wait_for(st.at[pl.ds(0, n_tp - 1)], send_sem.at[b, 0])
        wait_for(d_at(dn, me_x), send_sem.at[b, 1])
        wait_for(d_at(dn, me_x), send_sem.at[b, 2])
        wait_for(d_at(dn, x_left, 0, d_cut), send_sem.at[b, 3])
        wait_for(d_at(dn, x_right, d_cut, width - d_cut), send_sem.at[b, 4])
        flat = st.reshape(n_fs, *st.shape[2:])
        wait_for(flat.at[pl.ds(0, n_fs - 1)], send_sem.at[b, 5])
        wait_for(gu.at[:, :, me_x], send_sem.at[b, 6])
        wait_for(gu.at[:, :, me_x], send_sem.at[b, 7])
        wait_for(gu.at[:, :, me_x], send_sem.at[b, 8])
        wait_for(xch, send_sem.at[b, 9])
        wait_for(ring, send_sem.at[b, 10])
    wait_for(ring1, send_sem.at[0, 11])
    wait_for(xch1, send_sem.at[1, 11])


def body(prompt, gate_first, up_first, down_first, norm_gain, gate_second, up_second, down_second):
    n_fs, n_tp = lax.axis_size("fs"), lax.axis_size("tp")
    n_z, served = n_fs // 2, n_fs // n_tp
    half = n_z // 2
    features = prompt.shape[-1]
    own = prompt.shape[-2] // n_fs
    width = down_first.shape[0]
    wide = -(-width // LANES) * LANES
    bf16 = jnp.bfloat16
    row_block = gate_first.shape[0]
    gain_rows = lax.dynamic_slice_in_dim(norm_gain, lax.axis_index("fs") * row_block, row_block, 0)[:, None]

    src1 = pack_pair(gate_first.astype(bf16), up_first.astype(bf16), n_tp, served)
    src2 = pack_pair(
        (gain_rows * gate_second).astype(bf16), (gain_rows * up_second).astype(bf16), n_tp, served
    )
    tokens = prompt.reshape(n_z, 2, own, features)
    gu_shape = (n_z, 2, n_tp, row_block // n_tp, src1.shape[-1])
    hbm = pl.BlockSpec(memory_space=pltpu.HBM)
    vmem = pl.BlockSpec(memory_space=pltpu.VMEM)
    dma = pltpu.SemaphoreType.DMA
    result, gu1, gu2, down_one, down_two = pl.pallas_call(
        functools.partial(kernel, n_fs, n_tp, width),
        out_shape=[
            jax.ShapeDtypeStruct((own, features), bf16),
            jax.ShapeDtypeStruct(gu_shape, bf16),
            jax.ShapeDtypeStruct(gu_shape, bf16),
            jax.ShapeDtypeStruct((width, features), bf16),
            jax.ShapeDtypeStruct((width, features), bf16),
        ],
        in_specs=[hbm, vmem, hbm, hbm, hbm, hbm],
        out_specs=[vmem, hbm, hbm, hbm, hbm],
        scratch_shapes=[
            pltpu.VMEM((n_z, 2, own, features), bf16),
            pltpu.VMEM((n_z, 2, own, features), bf16),
            pltpu.VMEM(src1.shape, bf16),
            pltpu.VMEM(src1.shape, bf16),
            pltpu.VMEM(gu_shape, bf16),
            pltpu.VMEM(gu_shape, bf16),
            pltpu.VMEM((wide, features), bf16),
            pltpu.VMEM((wide, features), bf16),
            pltpu.VMEM((n_z, 2, own, features), bf16),
            pltpu.VMEM((n_z, 2, own, features), bf16),
            pltpu.VMEM((n_z, own, features), bf16),
            pltpu.VMEM((n_z, own, features), bf16),
            pltpu.VMEM((n_z - 1, own, features), bf16),
            pltpu.VMEM((n_z - 1, own, features), bf16),
            dma((5,)),
            dma((4,)),
            dma((2, n_tp - 1)),
            dma((2, n_z)),
            dma((2, 3, n_z)),
            dma((2, 4)),
            dma((2, n_z)),
            dma((2, 2, half, SUBS)),
            dma((2, half, SUBS)),
            dma((n_z,)),
            dma((2, 12)),
        ],
        compiler_params=pltpu.CompilerParams(
            collective_id=0, has_side_effects=True, vmem_limit_bytes=60 * 1024 * 1024
        ),
    )(tokens, norm_gain[None, :], src1, src2, down_first.astype(bf16), down_second.astype(bf16))
    gate_one, up_one = unpack_pair(gu1, width)
    gate_two, up_two = unpack_pair(gu2, width)
    return (result[None], gate_one, up_one, down_one, gate_two, up_two, down_two)


def solution(mesh):
    weight = P("fs", "tp")
    return jax.shard_map(
        body,
        mesh=mesh,
        in_specs=(P(("grp", "tp"), None, None), weight, weight, weight, P(), weight, weight, weight),
        out_specs=(
            P(("grp", "tp"), "fs", None),
            P("grp", "fs"),
            P("grp", "fs"),
            P("fs", "grp"),
            P("grp", "fs"),
            P("grp", "fs"),
            P("fs", "grp"),
        ),
        check_vma=False,
    )
```
